32 devices in a mesh: ep: 8 (over z, y), tp: 4 (over x, core).
Axes of the slice: x: 2, y: 2, z: 4, core: 2. Of those that a mesh axis runs over, the one named last changes fastest.
Arguments:
- tokens: bfloat16 [128, 2048], P('ep', 'tp'), may hold values from -40 to 40
- kv_cache: bfloat16 [128, 1024, 512], P('ep', None, 'tp'), may hold values from -1000 to 1000
- cum_gate: float32 [128, 16, 1024], P('ep', 'tp'), may hold values from -400 to 0, as said below
- lengths: int32 [128], P('ep'), may hold values from 256 to 1024
- w_query: bfloat16 [2048, 1024], P(None, 'tp'), may hold values from -0.125 to 0.125
- w_key: bfloat16 [2048, 256], P(None, 'tp'), may hold values from -0.125 to 0.125
- w_value: bfloat16 [2048, 256], P(None, 'tp'), may hold values from -0.125 to 0.125
- w_forget: bfloat16 [2048, 16], P(None, 'tp'), may hold values from -0.5 to 0.5
- forget_bias: float32 [16], P('tp'), may hold values from -2.5 to 1.5
- w_out: bfloat16 [1024, 2048], P('tp'), may hold values from -0.1875 to 0.1875
- attn_gain: bfloat16 [2048], replicated, may hold values from 0.099609375 to 1.8984375
- ffn_gain: bfloat16 [2048], replicated, may hold values from 0.099609375 to 1.8984375
- mix_gate: bfloat16 [2048], replicated, may hold values from -0.125 to 0.125
- expert_gate: bfloat16 [8, 2048, 1024], P('ep', None, 'tp'), may hold values from -0.125 to 0.125
- expert_up: bfloat16 [8, 2048, 1024], P('ep', None, 'tp'), may hold values from -0.125 to 0.125
- expert_down: bfloat16 [8, 1024, 2048], P('ep', 'tp'), may hold values from -0.1875 to 0.1875
- chosen: int32 [128, 2], P('ep'), may hold values from 0 to 7, as said below
- route_weight: float32 [128, 2], P('ep'), may hold values from 0.5 to 1.5
- dense_gate: bfloat16 [2048, 1024], P(None, 'tp'), may hold values from -0.125 to 0.125
- dense_up: bfloat16 [2048, 1024], P(None, 'tp'), may hold values from -0.125 to 0.125
- dense_down: bfloat16 [1024, 2048], P('tp'), may hold values from -0.1875 to 0.1875
Outputs:
- mixed: bfloat16 [128, 2048], P('ep', 'tp')
The draws below stay inside these ranges and needn't reach their ends.
Inputs may be any that keep to these rules, and one draw needn't show every extreme that they name: `cum_gate`: along positions each row never rises: entry p is the sum of the log forget gates of positions 0 to p of that sequence and head. `chosen`: each row names two different experts of one group of 8 consecutive expert numbers. The rows of one device name any one expert at most 8 times, and some expert exactly 8 times.
All inputs are finite; a program needn't handle non-finite values.
Results may differ from the reference program's by a relative error of at most 0.014.
Values may be sent and summed in bfloat16 or wider, within the bound.
No kernel may reach another device: no remote copies, remote signals or barrier semaphores. Data moves between devices by JAX's collectives and lax.ppermute only.
A program may use at most 64 MiB of HBM per device.

```python
import jax
import jax.numpy as jnp
from jax import lax

D = 2048
QUERY_HEADS = 16
KVH = 4
HD = 64
DE = 1024
DF = 1024
EPG = 8
TOP = 2
CACHED_POSITIONS = 1024
SEQ_DEV = 16
SEQUENCE_TOTAL = 128
EXPERTS = 8
CAP = 8
N_EP = 8
N_TP = 4


def draw_tokens(key, part):
    first, second, third = jax.random.split(key, 3)
    column_pos = jnp.arange(D, dtype=jnp.float32) / D
    entries = jax.random.normal(first, (SEQUENCE_TOTAL, D), jnp.float32)
    column_scale = 3.0 ** column_pos
    row_scale = jnp.exp(jax.random.uniform(second, (SEQUENCE_TOTAL, 1), jnp.float32, jnp.log(0.5), jnp.log(2.0)))
    roughness = jnp.exp(jax.random.uniform(third, (1, D), jnp.float32, jnp.log(0.5), jnp.log(2.0)))
    return (entries * 0.6 * column_scale[None, :] * roughness * row_scale).astype(jnp.bfloat16)


def draw_kv_cache(key, part):
    first = jax.random.fold_in(key, 0)
    total_width = 2 * KVH * HD
    entries = jax.random.normal(first, (SEQUENCE_TOTAL, CACHED_POSITIONS, total_width), jnp.float32)
    return entries.astype(jnp.bfloat16)


def draw_cum_gate(key, part):
    key_rows = jax.random.split(key, 7)
    scores_int = jax.random.randint(key_rows[0], (SEQUENCE_TOTAL, QUERY_HEADS), 0, 2 ** 20) * QUERY_HEADS + jnp.arange(QUERY_HEADS, dtype=jnp.int32)[None, :]
    ranking = jnp.argsort(jnp.argsort(scores_int, axis=1), axis=1)
    slow_count = QUERY_HEADS // 2
    slow = (ranking < slow_count)[:, :, None]
    slow_rate = jnp.exp(jax.random.uniform(key_rows[1], (SEQUENCE_TOTAL, QUERY_HEADS, 1), jnp.float32, jnp.log(0.2), jnp.log(0.8))) / CACHED_POSITIONS
    fast_rate = jnp.exp(jax.random.uniform(key_rows[2], (SEQUENCE_TOTAL, QUERY_HEADS, 1), jnp.float32, jnp.log(0.01), jnp.log(1.0 / 30.0)))
    rate_all = jnp.where(slow, slow_rate, fast_rate)
    block_factor = jnp.exp(jax.random.uniform(key_rows[3], (SEQUENCE_TOTAL, 1, CACHED_POSITIONS // 128), jnp.float32, jnp.log(0.5), jnp.log(2.0)))
    block_factor = jnp.repeat(block_factor, 128, axis=2)
    roughness = jnp.exp(jax.random.uniform(key_rows[4], (SEQUENCE_TOTAL, QUERY_HEADS, CACHED_POSITIONS), jnp.float32, jnp.log(0.5), jnp.log(2.0)))
    stepping_through = -rate_all * block_factor * roughness
    group_position = jax.random.randint(key_rows[5], (SEQUENCE_TOTAL, QUERY_HEADS, 2), 0, CACHED_POSITIONS)
    group_length = jnp.log(jax.random.uniform(key_rows[6], (SEQUENCE_TOTAL, QUERY_HEADS, 2), jnp.float32, 0.5, 0.8))
    position_rows = jnp.arange(CACHED_POSITIONS, dtype=jnp.int32)
    position_groups = jnp.sum(jnp.where(position_rows[None, None, None, :] == group_position[:, :, :, None], group_length[:, :, :, None], 0.0), axis=2)
    return jnp.cumsum(stepping_through + position_groups, axis=-1).astype(jnp.float32)


def draw_chosen(key, part):
    pair_count = EXPERTS // 2

    def one_block(block_key):
        key_perm, key_first, key_rest, key_order = jax.random.split(block_key, 4)
        group_keys = jax.random.split(key_perm, EXPERTS // EPG)

        def shuffle_group(group_key):
            return jax.random.permutation(group_key, EPG).astype(jnp.int32)
        shuffled = jax.vmap(shuffle_group)(group_keys)
        offsets = (jnp.arange(EXPERTS // EPG, dtype=jnp.int32) * EPG)[:, None]
        members = (shuffled + offsets).reshape(pair_count, 2).astype(jnp.int32)
        first_pair = jax.random.randint(key_first, (), 0, pair_count).astype(jnp.int32)
        others = (jax.random.permutation(key_rest, (pair_count - 1) * CAP)[:SEQ_DEV - CAP] // CAP).astype(jnp.int32)
        others = others + (others >= first_pair).astype(jnp.int32)
        pairs = jnp.concatenate([jnp.full((CAP,), first_pair, jnp.int32), others])
        pairs = pairs[jax.random.permutation(key_order, SEQ_DEV)]
        return members[pairs]
    block_keys = jax.random.split(key, N_EP)
    return jax.vmap(one_block)(block_keys).reshape(SEQ_DEV * N_EP, TOP).astype(jnp.int32)


def with_ends(result, rng, smallest, high):
    longest = result.shape.index(max(result.shape))
    spots = []
    for shift in (0, 1):
        where = [jax.random.randint(jax.random.fold_in(rng, axis), (), 0, length) for axis, length in enumerate(result.shape)]
        where[longest] = (where[longest] + shift) % result.shape[longest]
        spots.append(tuple(where))
    return result.at[spots[0]].set(smallest).at[spots[1]].set(high)


def level_of(own_key, extent, pieces, smallest, high):
    level, own = 1.0, jax.random.fold_in(own_key, 6)
    for axis_at, shards_of in pieces:
        draws = jnp.exp(jax.random.uniform(jax.random.fold_in(own, axis_at), (shards_of,), jnp.float32, smallest / len(pieces), high / len(pieces)))
        level = level * jnp.repeat(draws, extent[axis_at] // shards_of).reshape([-1 if axis == axis_at else 1 for axis in range(len(extent))])
    return level


def normal_values(own_key, extent, width, reach, cuts=(), kind=jnp.bfloat16):
    array = jax.random.normal(own_key, extent, jnp.float32) * width
    if len(cuts) > 0:
        array = level_of(own_key, extent, cuts, -0.22, 0.18) * array
    return jnp.clip(array, min=-reach, max=reach).astype(kind)


def setup_inputs(seed: int = 0) -> dict:
    key_of = jax.random.split(jax.random.key(seed), 22)
    tokens = draw_tokens(jax.random.fold_in(key_of[21], 71), 0)
    kv_cache = draw_kv_cache(jax.random.fold_in(key_of[21], 71), 0)
    cum_gate = draw_cum_gate(jax.random.fold_in(key_of[21], 71), 0)
    lengths = with_ends(jax.random.randint(key_of[3], (SEQUENCE_TOTAL,), CACHED_POSITIONS // 4, CACHED_POSITIONS + 1), jax.random.fold_in(key_of[3], 1), CACHED_POSITIONS // 4, CACHED_POSITIONS).astype(jnp.int32)
    w_query = normal_values(key_of[4], (D, QUERY_HEADS * HD), D ** -0.5, 0.125, ((1, 4),))
    w_key = normal_values(key_of[5], (D, KVH * HD), D ** -0.5, 0.125, ((1, 4),))
    w_value = normal_values(key_of[6], (D, KVH * HD), D ** -0.5, 0.125, ((1, 4),))
    w_forget = normal_values(key_of[7], (D, QUERY_HEADS), (D // 16) ** -0.5, 0.5, ((1, 4),))
    forget_bias = jnp.clip(-2.5 + 4.0 * jax.random.uniform(key_of[8], (QUERY_HEADS,), jnp.float32) ** level_of(key_of[8], (QUERY_HEADS,), ((0, 4),), -0.2, 0.2), -2.5, 1.5)
    w_out = normal_values(key_of[9], (QUERY_HEADS * HD, D), (QUERY_HEADS * HD) ** -0.5, 0.1875, ((0, 4),))
    attn_gain = jnp.clip(1.0 + 0.18 * jax.random.normal(key_of[10], (D,), jnp.float32), 0.099609375, 1.8984375).astype(jnp.bfloat16)
    ffn_gain = jnp.clip(1.0 + 0.18 * jax.random.normal(key_of[11], (D,), jnp.float32), 0.099609375, 1.8984375).astype(jnp.bfloat16)
    mix_gate = normal_values(key_of[12], (D,), D ** -0.5, 0.125)
    expert_gate = normal_values(key_of[13], (EXPERTS, D, DE), D ** -0.5, 0.125, ((0, 8), (2, 4)))
    expert_up = normal_values(key_of[14], (EXPERTS, D, DE), D ** -0.5, 0.125, ((0, 8), (2, 4)))
    expert_down = normal_values(key_of[15], (EXPERTS, DE, D), DE ** -0.5, 0.1875, ((0, 8), (1, 4)))
    chosen = draw_chosen(jax.random.fold_in(key_of[21], 71), 0)
    route_weight = jnp.clip(0.5 + 1.0 * jax.random.uniform(key_of[17], (SEQUENCE_TOTAL, TOP), jnp.float32) ** level_of(key_of[17], (SEQUENCE_TOTAL, TOP), ((0, 8),), -0.2, 0.2), 0.5, 1.5)
    dense_gate = normal_values(key_of[18], (D, DF), D ** -0.5, 0.125, ((1, 4),))
    dense_up = normal_values(key_of[19], (D, DF), D ** -0.5, 0.125, ((1, 4),))
    dense_down = normal_values(key_of[20], (DF, D), DF ** -0.5, 0.1875, ((0, 4),))
    return {"tokens": tokens, "kv_cache": kv_cache, "cum_gate": cum_gate, "lengths": lengths, "w_query": w_query, "w_key": w_key, "w_value": w_value, "w_forget": w_forget, "forget_bias": forget_bias, "w_out": w_out, "attn_gain": attn_gain, "ffn_gain": ffn_gain, "mix_gate": mix_gate, "expert_gate": expert_gate, "expert_up": expert_up, "expert_down": expert_down, "chosen": chosen, "route_weight": route_weight, "dense_gate": dense_gate, "dense_up": dense_up, "dense_down": dense_down}


epsilon = 1e-06

def norm_rows(values, scales):
    widened = values.astype(jnp.float32)
    square = lax.optimization_barrier(jnp.mean(widened * widened, axis=-1, keepdims=True))
    return (widened * lax.rsqrt(square + epsilon) * scales.astype(jnp.float32)).astype(jnp.bfloat16)

def split_sum(left, right):
    piece_width = left.shape[1] // N_TP
    running = jnp.zeros((left.shape[0], right.shape[1]), jnp.float32)
    for member in range(N_TP):
        lower = member * piece_width
        partial_value = jnp.dot(left[:, lower:lower + piece_width], right[lower:lower + piece_width], preferred_element_type=jnp.float32).astype(jnp.bfloat16)
        partial_value = lax.optimization_barrier(partial_value)
        running = running + partial_value.astype(jnp.float32)
    return running

def reference(tokens, kv_cache, cum_gate, lengths, w_query, w_key, w_value, w_forget, forget_bias, w_out, attn_gain, ffn_gain, mix_gate, expert_gate, expert_up, expert_down, chosen, route_weight, dense_gate, dense_up, dense_down):
    group_size = QUERY_HEADS // KVH
    score_scale = HD ** (-0.5)
    h_one = norm_rows(tokens, attn_gain)
    queries = jnp.dot(h_one, w_query, preferred_element_type=jnp.float32).astype(jnp.bfloat16)
    key_new = jnp.dot(h_one, w_key, preferred_element_type=jnp.float32).astype(jnp.bfloat16)
    value_new = jnp.dot(h_one, w_value, preferred_element_type=jnp.float32).astype(jnp.bfloat16)
    log_forget = jax.nn.log_sigmoid(jnp.dot(h_one, w_forget, preferred_element_type=jnp.float32) + forget_bias)

    def one_sequence(packed):
        query_row, key_row, value_row, forget_row, cache_row, gate_row, length_one = packed
        query_heads = query_row.astype(jnp.float32).reshape(KVH, group_size, HD)
        stacked = cache_row.astype(jnp.float32).reshape(CACHED_POSITIONS, KVH, 2, HD)
        scores = jnp.einsum('jgd,cjd->jgc', query_heads, stacked[:, :, 0, :]) * score_scale
        gate_rows = gate_row.reshape(KVH, group_size, CACHED_POSITIONS)
        latest = lax.dynamic_index_in_dim(gate_rows, (length_one - 1).astype(jnp.int32), axis=2, keepdims=True)
        scores = scores + latest - gate_rows + forget_row.reshape(KVH, group_size)[:, :, None]
        position_rows = jnp.arange(CACHED_POSITIONS, dtype=jnp.int32)
        scores = jnp.where(position_rows[None, None, :] < length_one, scores, -jnp.inf)
        own_score = jnp.einsum('jgd,jd->jg', query_heads, key_row.astype(jnp.float32).reshape(KVH, HD)) * score_scale
        highest = jnp.maximum(lax.optimization_barrier(jnp.max(scores, axis=-1)), own_score)
        weights = jnp.exp(scores - highest[:, :, None])
        own_weight = jnp.exp(own_score - highest)
        denominator = lax.optimization_barrier(jnp.sum(weights, axis=-1)) + own_weight
        weights = (weights / denominator[:, :, None]).astype(jnp.bfloat16)
        own_weight = (own_weight / denominator).astype(jnp.bfloat16)
        blended = jnp.einsum('jgc,cjd->jgd', weights.astype(jnp.float32), stacked[:, :, 1, :])
        blended = blended + own_weight.astype(jnp.float32)[:, :, None] * value_row.astype(jnp.float32).reshape(KVH, 1, HD)
        return blended.astype(jnp.bfloat16).reshape(QUERY_HEADS * HD)
    head_out = lax.map(one_sequence, (queries, key_new, value_new, log_forget, kv_cache, cum_gate, lengths))
    attention = split_sum(head_out, w_out)
    residual = (tokens.astype(jnp.float32) + attention).astype(jnp.bfloat16)
    h_two = norm_rows(residual, ffn_gain)
    flat_routes = chosen.reshape(N_EP, SEQ_DEV * TOP)
    one_hot = (flat_routes[:, :, None] == jnp.arange(EXPERTS, dtype=jnp.int32)[None, None, :]).astype(jnp.int32)
    earlier = (jnp.cumsum(one_hot, axis=1) - one_hot).astype(jnp.int32)
    rank_of = lax.optimization_barrier(jnp.sum(earlier * one_hot, axis=-1)).astype(jnp.int32)
    slot_of = (jnp.arange(N_EP, dtype=jnp.int32)[:, None] * CAP + rank_of).reshape(-1).astype(jnp.int32)
    expert_of = flat_routes.reshape(-1).astype(jnp.int32)
    source_rows = (jnp.arange(SEQUENCE_TOTAL * TOP, dtype=jnp.int32) // TOP).astype(jnp.int32)
    buffer = jnp.zeros((EXPERTS, N_EP * CAP, D), jnp.bfloat16).at[expert_of, slot_of].set(h_two[source_rows])

    def run_expert(packed):
        inputs_here, gate_here, up_here, down_here = packed
        gate_pre = jnp.dot(inputs_here, gate_here, preferred_element_type=jnp.float32)
        up_pre = jnp.dot(inputs_here, up_here, preferred_element_type=jnp.float32)
        hidden = (jax.nn.silu(gate_pre) * up_pre).astype(jnp.bfloat16)
        return split_sum(hidden, down_here).astype(jnp.bfloat16)
    expert_rows = lax.map(run_expert, (buffer, expert_gate, expert_up, expert_down))
    picked = expert_rows[expert_of, slot_of].astype(jnp.float32).reshape(SEQUENCE_TOTAL, TOP, D)
    routed_sum = lax.optimization_barrier(jnp.sum(picked * route_weight[:, :, None], axis=1))
    dense_pre = jnp.dot(h_two, dense_gate, preferred_element_type=jnp.float32)
    dense_lift = jnp.dot(h_two, dense_up, preferred_element_type=jnp.float32)
    dense_act = (jax.nn.silu(dense_pre) * dense_lift).astype(jnp.bfloat16)
    dense_out = split_sum(dense_act, dense_down)
    blend_gate = jax.nn.sigmoid(jnp.dot(h_two, mix_gate, preferred_element_type=jnp.float32))
    return (residual.astype(jnp.float32) + routed_sum + blend_gate[:, None] * dense_out).astype(jnp.bfloat16)
```

```python
import jax
import jax.numpy as jnp
from jax import lax
from jax.sharding import PartitionSpec as P

HD = 64
TOP = 2


epsilon = 1e-06


def norm_rows(values, scales):
    widened = values.astype(jnp.float32)
    square = jnp.mean(widened * widened, axis=-1, keepdims=True)
    return (widened * lax.rsqrt(square + epsilon) * scales.astype(jnp.float32)).astype(jnp.bfloat16)


def attend(h_one, kv_cache, cum_gate, lengths, w_query, w_key, w_value, w_forget, forget_bias):
    tok_count = h_one.shape[0]
    cache_len = kv_cache.shape[1]
    kv_local = w_key.shape[1] // HD
    q_local = w_query.shape[1] // HD
    group_size = q_local // kv_local
    score_scale = HD ** (-0.5)
    queries = jnp.dot(h_one, w_query, preferred_element_type=jnp.float32).astype(jnp.bfloat16)
    queries = queries.reshape(tok_count, kv_local, group_size, HD)
    key_new = jnp.dot(h_one, w_key, preferred_element_type=jnp.float32).astype(jnp.bfloat16)
    key_new = key_new.reshape(tok_count, kv_local, HD)
    value_new = jnp.dot(h_one, w_value, preferred_element_type=jnp.float32).astype(jnp.bfloat16)
    value_new = value_new.reshape(tok_count, kv_local, HD)
    forget_now = jax.nn.log_sigmoid(
        jnp.dot(h_one, w_forget, preferred_element_type=jnp.float32) + forget_bias
    )
    forget_now = forget_now.reshape(tok_count, kv_local, group_size)
    stacked = kv_cache.reshape(tok_count, cache_len, kv_local, 2, HD)
    past_keys = stacked[:, :, :, 0, :]
    past_values = stacked[:, :, :, 1, :]
    scores = (
        jnp.einsum("sjgd,scjd->sjgc", queries, past_keys, preferred_element_type=jnp.float32)
        * score_scale
    )
    cumulative = cum_gate.reshape(tok_count, kv_local, group_size, cache_len)
    position_rows = jnp.arange(cache_len, dtype=jnp.int32)
    at_last = (position_rows[None, :] == (lengths - 1)[:, None]).astype(jnp.float32)
    latest = jnp.sum(cumulative * at_last[:, None, None, :], axis=-1, keepdims=True)
    scores = scores + latest - cumulative + forget_now[:, :, :, None]
    inside = position_rows[None, :] < lengths[:, None]
    scores = jnp.where(inside[:, None, None, :], scores, -jnp.inf)
    own_score = (
        jnp.einsum("sjgd,sjd->sjg", queries, key_new, preferred_element_type=jnp.float32)
        * score_scale
    )
    highest = jnp.maximum(jnp.max(scores, axis=-1), own_score)
    weights = jnp.exp(scores - highest[:, :, :, None])
    own_weight = jnp.exp(own_score - highest)
    denominator = jnp.sum(weights, axis=-1) + own_weight
    weights = (weights / denominator[:, :, :, None]).astype(jnp.bfloat16)
    own_weight = (own_weight / denominator).astype(jnp.bfloat16)
    blended = jnp.einsum(
        "sjgc,scjd->sjgd", weights, past_values, preferred_element_type=jnp.float32
    )
    blended = (
        blended
        + own_weight.astype(jnp.float32)[:, :, :, None]
        * value_new.astype(jnp.float32)[:, :, None, :]
    )
    return blended.astype(jnp.bfloat16).reshape(tok_count, q_local * HD)


def scatter_sum(part, axis):
    count = lax.axis_size(axis)
    width = part.shape[1] // count
    here = lax.axis_index(axis)
    total = lax.dynamic_slice_in_dim(part, here * width, width, 1).astype(jnp.float32)
    for step in range(1, count):
        goal = (here + step) % count
        block = lax.dynamic_slice_in_dim(part, goal * width, width, 1)
        moved = lax.ppermute(block, axis, [(i, (i + step) % count) for i in range(count)])
        total = total + moved.astype(jnp.float32)
    return total


def local(
    tokens,
    kv_cache,
    cum_gate,
    lengths,
    w_query,
    w_key,
    w_value,
    w_forget,
    forget_bias,
    w_out,
    attn_gain,
    ffn_gain,
    mix_gate,
    expert_gate,
    expert_up,
    expert_down,
    chosen,
    route_weight,
    dense_gate,
    dense_up,
    dense_down,
):
    tok_count = tokens.shape[0]
    slice_width = tokens.shape[1]
    ep_count = lax.axis_size("ep")
    gathered = lax.all_gather(tokens, "tp", axis=1, tiled=True)
    model_width = gathered.shape[1]
    h_one = norm_rows(gathered, attn_gain)
    head_out = attend(
        h_one, kv_cache, cum_gate, lengths, w_query, w_key, w_value, w_forget, forget_bias
    )
    partial_value = jnp.dot(head_out, w_out, preferred_element_type=jnp.float32)
    tp_offset = lax.axis_index("tp") * slice_width
    shared = lax.all_gather(partial_value.astype(jnp.bfloat16), "tp", axis=0)
    attention = jnp.sum(shared.astype(jnp.float32), axis=0)
    residual_full = (gathered.astype(jnp.float32) + attention).astype(jnp.bfloat16)
    h_two = norm_rows(residual_full, ffn_gain)
    residual = lax.dynamic_slice_in_dim(residual_full, tp_offset, slice_width, 1)
    capacity = max(2, (4 * tok_count + ep_count - 1) // ep_count)
    routes = chosen.reshape(-1)
    expert_ids = jnp.arange(ep_count, dtype=jnp.int32)
    one_hot = (routes[:, None] == expert_ids[None, :]).astype(jnp.int32)
    rank_of = jnp.sum((jnp.cumsum(one_hot, axis=0) - one_hot) * one_hot, axis=1)
    slot_of = routes * capacity + rank_of
    slot_ids = jnp.arange(ep_count * capacity, dtype=jnp.int32)
    chooser = (slot_ids[:, None] == slot_of[None, :]).astype(jnp.bfloat16)
    per_token = jnp.sum(chooser.reshape(ep_count * capacity, tok_count, TOP), axis=2)
    outgoing = jnp.dot(per_token, h_two, preferred_element_type=jnp.float32).astype(jnp.bfloat16)
    outgoing = outgoing.reshape(ep_count, capacity, model_width)
    received = lax.all_to_all(outgoing, "ep", split_axis=0, concat_axis=0, tiled=True)

    dense_pre = jnp.dot(h_two, dense_gate, preferred_element_type=jnp.float32)
    dense_lift = jnp.dot(h_two, dense_up, preferred_element_type=jnp.float32)
    dense_act = (jax.nn.silu(dense_pre) * dense_lift).astype(jnp.bfloat16)
    dense_part = jnp.dot(dense_act, dense_down, preferred_element_type=jnp.float32)
    dense_out = scatter_sum(dense_part.astype(jnp.bfloat16), "tp")
    blend_gate = jax.nn.sigmoid(jnp.dot(h_two, mix_gate, preferred_element_type=jnp.float32))

    flat_rows = received.reshape(-1, model_width)
    gate_pre = jnp.dot(flat_rows, expert_gate[0], preferred_element_type=jnp.float32)
    up_pre = jnp.dot(flat_rows, expert_up[0], preferred_element_type=jnp.float32)
    hidden = (jax.nn.silu(gate_pre) * up_pre).astype(jnp.bfloat16)
    part_out = jnp.dot(hidden, expert_down[0], preferred_element_type=jnp.float32)
    tp_count = lax.axis_size("tp")
    parts = part_out.astype(jnp.bfloat16).reshape(ep_count, capacity, tp_count, slice_width)
    parts = parts.transpose(0, 2, 1, 3).reshape(ep_count * tp_count, capacity, slice_width)
    returned = lax.all_to_all(parts, ("ep", "tp"), split_axis=0, concat_axis=0, tiled=True)
    returned = returned.reshape(ep_count, tp_count, capacity, slice_width).astype(jnp.float32)
    returned = jnp.sum(returned, axis=1).astype(jnp.bfloat16)
    returned = returned.reshape(ep_count * capacity, slice_width)
    picked = jnp.dot(chooser.T, returned, preferred_element_type=jnp.float32)
    routed_sum = jnp.sum(
        picked.reshape(tok_count, TOP, slice_width) * route_weight[:, :, None], axis=1
    )
    return (residual.astype(jnp.float32) + routed_sum + blend_gate[:, None] * dense_out).astype(
        jnp.bfloat16
    )


def solution(mesh):
    in_specs = (
        P("ep", "tp"),
        P("ep", None, "tp"),
        P("ep", "tp", None),
        P("ep"),
        P(None, "tp"),
        P(None, "tp"),
        P(None, "tp"),
        P(None, "tp"),
        P("tp"),
        P("tp", None),
        P(),
        P(),
        P(),
        P("ep", None, "tp"),
        P("ep", None, "tp"),
        P("ep", "tp", None),
        P("ep", None),
        P("ep", None),
        P(None, "tp"),
        P(None, "tp"),
        P("tp", None),
    )
    out_specs = P("ep", "tp")
    return jax.shard_map(local, mesh=mesh, in_specs=in_specs, out_specs=out_specs, check_vma=False)
```

```python
import jax
import jax.numpy as jnp
from jax import lax
from jax.experimental import pallas as pl
from jax.experimental.pallas import tpu as pltpu
from jax.sharding import PartitionSpec as P

HD = 64
TOP = 2


epsilon = 1e-06


def norm_rows(values, scales):
    widened = values.astype(jnp.float32)
    square = jnp.mean(widened * widened, axis=-1, keepdims=True)
    return (widened * lax.rsqrt(square + epsilon) * scales.astype(jnp.float32)).astype(jnp.bfloat16)


NT = (((1,), (1,)), ((), ()))

def attend_kernel(x_ref, gain_ref, wq_ref, wk_ref, wv_ref, wf_ref, bias_ref, len_ref, cum_ref, kv_ref, wo_ref,
                  out_ref, q_scr, e_scr, p_scr, o_scr):
    f32, bf16 = jnp.float32, jnp.bfloat16
    tok = x_ref.shape[0]
    group = cum_ref.shape[1]
    cache = kv_ref.shape[1]
    pack = 8 // group
    rows = pack * group
    x = x_ref[...].astype(f32)
    square = jnp.mean(x * x, axis=1, keepdims=True)
    h = (x * lax.rsqrt(square + epsilon) * gain_ref[...].astype(f32)).astype(bf16)
    q = jnp.dot(h, wq_ref[...], preferred_element_type=f32).astype(bf16).astype(f32)
    k_new = lax.dot_general(h, wk_ref[...], NT, preferred_element_type=f32).astype(bf16).astype(f32)
    v_new = lax.dot_general(h, wv_ref[...], NT, preferred_element_type=f32).astype(bf16).astype(f32)
    forget = lax.dot_general(h, wf_ref[...], NT, preferred_element_type=f32) + bias_ref[...]
    forget = jnp.minimum(forget, 0.0) - jnp.log1p(jnp.exp(-jnp.abs(forget)))
    scale = HD ** (-0.5)
    lane = lax.broadcasted_iota(jnp.int32, (tok, 2 * HD), 1)
    for g in range(group):
        qg = q[:, g * HD:(g + 1) * HD]
        own = jnp.sum(qg * k_new, axis=1, keepdims=True) * scale
        q_scr[pl.ds(g, tok, stride=group), :] = jnp.concatenate([qg * scale, jnp.zeros_like(qg)], axis=1)
        e_scr[pl.ds(g, tok, stride=group), :] = jnp.where(lane == 0, forget[:, g:g + 1], own)
    row = lax.broadcasted_iota(jnp.int32, (rows, cache), 0)
    column = lax.broadcasted_iota(jnp.int32, (rows, cache), 1)
    small = lax.broadcasted_iota(jnp.int32, (rows, 2 * HD), 0)
    for b in range(tok // pack):
        qb = q_scr[b * rows:(b + 1) * rows, :].astype(bf16)
        s = lax.dot_general(qb, kv_ref[b * pack], NT, preferred_element_type=f32)
        used = jnp.full((rows, cache), len_ref[b * pack], jnp.int32)
        for j in range(1, pack):
            sj = lax.dot_general(qb, kv_ref[b * pack + j], NT, preferred_element_type=f32)
            s = jnp.where(row < j * group, s, sj)
            used = jnp.where(row < j * group, used, len_ref[b * pack + j])
        cum = jnp.concatenate([cum_ref[b * pack + j] for j in range(pack)], axis=0)
        extra = e_scr[b * rows:(b + 1) * rows, :]
        own = extra[:, 1:2]
        latest = jnp.sum(jnp.where(column == used - 1, cum, 0.0), axis=1, keepdims=True)
        s = s + (latest + extra[:, 0:1]) - cum
        s = jnp.where(column < used, s, -jnp.inf)
        top = jnp.maximum(jnp.max(s, axis=1, keepdims=True), own)
        w = jnp.exp(s - top)
        own_w = jnp.exp(own - top)
        inv = 1.0 / (jnp.sum(w, axis=1, keepdims=True) + own_w)
        p = (w * inv).astype(bf16)
        o = jnp.dot(p, kv_ref[b * pack], preferred_element_type=f32)
        for j in range(1, pack):
            oj = jnp.dot(p, kv_ref[b * pack + j], preferred_element_type=f32)
            o = jnp.where(small < j * group, o, oj)
        o_scr[b * rows:(b + 1) * rows, :] = o
        p_scr[b * rows:(b + 1) * rows, :] = jnp.broadcast_to((own_w * inv).astype(bf16).astype(f32), (rows, 2 * HD))
    heads = []
    for g in range(group):
        o = o_scr[pl.ds(g, tok, stride=group), :][:, HD:]
        w = p_scr[pl.ds(g, tok, stride=group), :][:, HD:]
        heads.append((o + w * v_new).astype(bf16))
    head_out = jnp.concatenate(heads, axis=1)
    out_ref[...] = jnp.dot(head_out, wo_ref[...], preferred_element_type=f32).astype(bf16)


def attend(x, kv_cache, cum_gate, lengths, w_query, w_key, w_value, w_forget, forget_bias, w_out, gain):
    tok = x.shape[0]
    group = cum_gate.shape[1]
    vmem = pl.BlockSpec(memory_space=pltpu.VMEM)
    smem = pl.BlockSpec(memory_space=pltpu.SMEM)
    scr = pltpu.VMEM((tok * group, 2 * HD), jnp.float32)
    return pl.pallas_call(
        attend_kernel,
        out_shape=jax.ShapeDtypeStruct((tok, w_out.shape[1]), jnp.bfloat16),
        in_specs=[vmem] * 7 + [smem] + [vmem] * 3,
        out_specs=vmem,
        scratch_shapes=[scr] * 4,
        compiler_params=pltpu.CompilerParams(vmem_limit_bytes=16 << 20),
        name="attend",
    )(x, gain.reshape(1, -1), w_query, w_key.T, w_value.T, w_forget.T, forget_bias.reshape(1, -1), lengths, cum_gate,
      kv_cache, w_out)


def expert_kernel(x_ref, wg_ref, wu_ref, wd_ref, out_ref):
    f32, bf16 = jnp.float32, jnp.bfloat16
    x = x_ref[...]
    a = jnp.dot(x, wg_ref[...], preferred_element_type=f32)
    b = jnp.dot(x, wu_ref[...], preferred_element_type=f32)
    hidden = (a / (1.0 + jnp.exp(-a)) * b).astype(bf16)
    y = jnp.dot(hidden, wd_ref[...], preferred_element_type=f32).astype(bf16)
    width = out_ref.shape[3]
    cap = out_ref.shape[2]
    for t in range(out_ref.shape[1]):
        out_ref[:, t] = y[:, t * width:(t + 1) * width].reshape(-1, cap, width)


def expert(x, wg, wu, wd, ep, tp, cap):
    return pl.pallas_call(
        expert_kernel,
        out_shape=jax.ShapeDtypeStruct((ep, tp, cap, wd.shape[1] // tp), jnp.bfloat16),
        compiler_params=pltpu.CompilerParams(vmem_limit_bytes=16 << 20),
        name="expert",
    )(x, wg, wu, wd)


def scatter_sum(part, axis):
    count = lax.axis_size(axis)
    width = part.shape[1] // count
    here = lax.axis_index(axis)
    total = lax.dynamic_slice_in_dim(part, here * width, width, 1).astype(jnp.float32)
    for step in range(1, count):
        goal = (here + step) % count
        block = lax.dynamic_slice_in_dim(part, goal * width, width, 1)
        moved = lax.ppermute(block, axis, [(i, (i + step) % count) for i in range(count)])
        total = total + moved.astype(jnp.float32)
    return total


def local(
    tokens,
    kv_cache,
    cum_gate,
    lengths,
    w_query,
    w_key,
    w_value,
    w_forget,
    forget_bias,
    w_out,
    attn_gain,
    ffn_gain,
    mix_gate,
    expert_gate,
    expert_up,
    expert_down,
    chosen,
    route_weight,
    dense_gate,
    dense_up,
    dense_down,
):
    tok_count = tokens.shape[0]
    slice_width = tokens.shape[1]
    ep_count = lax.axis_size("ep")
    gathered = lax.all_gather(tokens, "tp", axis=1, tiled=True)
    model_width = gathered.shape[1]
    partial_value = attend(
        gathered,
        kv_cache,
        cum_gate,
        lengths,
        w_query,
        w_key,
        w_value,
        w_forget,
        forget_bias,
        w_out,
        attn_gain,
    )
    tp_offset = lax.axis_index("tp") * slice_width
    shared = lax.all_gather(partial_value, "tp", axis=0)
    attention = jnp.sum(shared.astype(jnp.float32), axis=0)
    residual_full = (gathered.astype(jnp.float32) + attention).astype(jnp.bfloat16)
    h_two = norm_rows(residual_full, ffn_gain)
    residual = lax.dynamic_slice_in_dim(residual_full, tp_offset, slice_width, 1)
    capacity = max(2, (4 * tok_count + ep_count - 1) // ep_count)
    routes = chosen.reshape(-1)
    expert_ids = jnp.arange(ep_count, dtype=jnp.int32)
    one_hot = (routes[:, None] == expert_ids[None, :]).astype(jnp.int32)
    rank_of = jnp.sum((jnp.cumsum(one_hot, axis=0) - one_hot) * one_hot, axis=1)
    slot_of = routes * capacity + rank_of
    slot_ids = jnp.arange(ep_count * capacity, dtype=jnp.int32)
    chooser = (slot_ids[:, None] == slot_of[None, :]).astype(jnp.bfloat16)
    per_token = jnp.sum(chooser.reshape(ep_count * capacity, tok_count, TOP), axis=2)
    outgoing = jnp.dot(per_token, h_two, preferred_element_type=jnp.float32).astype(jnp.bfloat16)
    outgoing = outgoing.reshape(ep_count, capacity, model_width)
    received = lax.all_to_all(outgoing, "ep", split_axis=0, concat_axis=0, tiled=True)

    dense_pre = jnp.dot(h_two, dense_gate, preferred_element_type=jnp.float32)
    dense_lift = jnp.dot(h_two, dense_up, preferred_element_type=jnp.float32)
    dense_act = (jax.nn.silu(dense_pre) * dense_lift).astype(jnp.bfloat16)
    dense_part = jnp.dot(dense_act, dense_down, preferred_element_type=jnp.float32)
    dense_out = scatter_sum(dense_part.astype(jnp.bfloat16), "tp")
    blend_gate = jax.nn.sigmoid(jnp.dot(h_two, mix_gate, preferred_element_type=jnp.float32))

    flat_rows = received.reshape(-1, model_width)
    tp_count = lax.axis_size("tp")
    parts = expert(
        flat_rows, expert_gate[0], expert_up[0], expert_down[0], ep_count, tp_count, capacity
    )
    parts = parts.reshape(ep_count * tp_count, capacity, slice_width)
    returned = lax.all_to_all(parts, ("ep", "tp"), split_axis=0, concat_axis=0, tiled=True)
    returned = returned.reshape(ep_count, tp_count, capacity, slice_width).astype(jnp.float32)
    returned = jnp.sum(returned, axis=1).astype(jnp.bfloat16)
    returned = returned.reshape(ep_count * capacity, slice_width)
    picked = jnp.dot(chooser.T, returned, preferred_element_type=jnp.float32)
    routed_sum = jnp.sum(
        picked.reshape(tok_count, TOP, slice_width) * route_weight[:, :, None], axis=1
    )
    return (residual.astype(jnp.float32) + routed_sum + blend_gate[:, None] * dense_out).astype(
        jnp.bfloat16
    )


def solution(mesh):
    in_specs = (
        P("ep", "tp"),
        P("ep", None, "tp"),
        P("ep", "tp", None),
        P("ep"),
        P(None, "tp"),
        P(None, "tp"),
        P(None, "tp"),
        P(None, "tp"),
        P("tp"),
        P("tp", None),
        P(),
        P(),
        P(),
        P("ep", None, "tp"),
        P("ep", None, "tp"),
        P("ep", "tp", None),
        P("ep", None),
        P("ep", None),
        P(None, "tp"),
        P(None, "tp"),
        P("tp", None),
    )
    out_specs = P("ep", "tp")
    return jax.shard_map(local, mesh=mesh, in_specs=in_specs, out_specs=out_specs, check_vma=False)
```

```python
import jax
import jax.numpy as jnp
from jax import lax
from jax.experimental import pallas as pl
from jax.experimental.pallas import tpu as pltpu
from jax.sharding import PartitionSpec as P

HD = 64
epsilon = 1e-06
f32, bf16 = jnp.float32, jnp.bfloat16
NT = (((1,), (1,)), ((), ()))
VM = pl.BlockSpec(memory_space=pltpu.VMEM)
HB = pl.BlockSpec(memory_space=pltpu.HBM)


def stay(*arrays):
    return [pltpu.with_memory_space_constraint(a, pltpu.HBM) for a in arrays]


def params(mib):
    return pltpu.CompilerParams(vmem_limit_bytes=mib << 20)


def row_of(ref):
    rows = ref[...].astype(f32)
    return jnp.concatenate([rows[i : i + 1] for i in range(rows.shape[0])], axis=1)


def prep_kernel(
    len_hbm, fb_hbm, gain_hbm, gain_two_hbm, mix_hbm, chosen_hbm, rw_hbm,
    cum_hbm, kv_hbm, wq_hbm, wk_hbm, wv_hbm, wf_hbm, wo_hbm,
    kv_ref, wq_ref, wkv_ref, wf_ref, wo_ref, bias_ref, gains_ref, send_ref, take_ref,
    len_ref, fb_ref, gain_ref, chosen_ref, rw_ref, cum_ref, sems,
    *, capacity, ep_count, tp_count,
):
    hd = wk_hbm.shape[0]
    moves = [
        (len_hbm, len_ref),
        (cum_hbm, cum_ref),
        (fb_hbm, fb_ref),
        (gain_hbm, gain_ref.at[0]),
        (gain_two_hbm, gain_ref.at[1]),
        (mix_hbm, gain_ref.at[2]),
        (chosen_hbm, chosen_ref),
        (rw_hbm, rw_ref),
        (wq_hbm, wq_ref),
        (wk_hbm, wkv_ref.at[pl.ds(0, hd)]),
        (wv_hbm, wkv_ref.at[pl.ds(hd, hd)]),
        (wf_hbm, wf_ref),
        (kv_hbm, kv_ref),
        (wo_hbm, wo_ref),
    ]
    copies = [pltpu.make_async_copy(a, b, sems.at[i]) for i, (a, b) in enumerate(moves)]
    for c in copies:
        c.start()
    tok, group, cache = cum_ref.shape
    pack = 8 // group
    rows = pack * group
    for c in copies[:8]:
        c.wait()
    row = lax.broadcasted_iota(jnp.int32, (rows, cache), 0)
    column = lax.broadcasted_iota(jnp.int32, (rows, cache), 1)
    for b in range(tok // pack):
        used = jnp.full((rows, cache), len_ref[b * pack], jnp.int32)
        for j in range(1, pack):
            used = jnp.where(row < j * group, used, len_ref[b * pack + j])
        cum = jnp.concatenate([cum_ref[b * pack + j] for j in range(pack)], axis=0)
        latest = jnp.sum(jnp.where(column == used - 1, cum, 0.0), axis=1, keepdims=True)
        bias_ref[b * rows : (b + 1) * rows, :] = jnp.where(column < used, latest - cum, -jnp.inf)
    width = gains_ref.shape[1]
    for i in range(3):
        gains_ref[i : i + 1, :] = row_of(gain_ref.at[i])
    spot = lax.broadcasted_iota(jnp.int32, (1, width), 1)
    biases = jnp.zeros((1, width), f32)
    for g in range(group):
        biases = jnp.where(spot == g, fb_ref[g], biases)
    gains_ref[3:4, :] = biases

    slots = ep_count * capacity
    expert_of = lax.broadcasted_iota(jnp.int32, (slots, tok), 0) // capacity
    place = lax.broadcasted_iota(jnp.int32, (slots, tok), 0) % capacity
    goes = (chosen_ref[0:1, :] == expert_of) | (chosen_ref[1:2, :] == expert_of)
    before = lax.broadcasted_iota(jnp.int32, (tok, tok), 0) < lax.broadcasted_iota(jnp.int32, (tok, tok), 1)
    rank = jnp.dot(goes.astype(f32), before.astype(f32), preferred_element_type=f32)
    send_ref[...] = jnp.where(goes & (rank == place.astype(f32)), 1.0, 0.0).astype(bf16)

    spread = (tok, slots * tp_count)
    side = lax.broadcasted_iota(jnp.int32, spread, 1)
    expert_of = side // (capacity * tp_count)
    place = side % capacity
    columns = jnp.concatenate([chosen_ref[...].astype(f32), rw_ref[...], jnp.zeros((4, tok), f32)], axis=0)
    columns = jnp.concatenate([columns, jnp.zeros((8, 128 - tok), f32)], axis=1).T[:tok]
    first = columns[:, 0:1] == expert_of.astype(f32)
    second = columns[:, 1:2] == expert_of.astype(f32)
    after = lax.broadcasted_iota(jnp.int32, (tok, tok), 1) < lax.broadcasted_iota(jnp.int32, (tok, tok), 0)
    goes = first | second
    rank = jnp.dot(after.astype(f32), goes.astype(f32), preferred_element_type=f32)
    weight = jnp.where(first, columns[:, 2:3], columns[:, 3:4])
    weight = jnp.where(goes & (rank == place.astype(f32)), weight, 0.0)
    upper = weight.astype(bf16)
    take_ref[0:tok, :] = upper
    take_ref[tok:, :] = (weight - upper.astype(f32)).astype(bf16)
    for c in copies[8:]:
        c.wait()


def prep(
    tokens, kv_cache, cum_gate, lengths, w_query, w_key, w_value, w_forget, forget_bias, w_out,
    attn_gain, ffn_gain, mix_gate, chosen, route_weight, capacity, ep_count, tp_count,
):
    tok, group, cache = cum_gate.shape
    width = w_query.shape[0]
    slots = ep_count * capacity
    outs = [
        (kv_cache.shape, bf16),
        (w_query.shape, bf16),
        ((2 * HD, width), bf16),
        ((group, width), bf16),
        (w_out.shape, bf16),
        ((tok * group, cache), f32),
        ((8, width), f32),
        ((slots, tok), bf16),
        ((2 * tok, slots * tp_count), bf16),
    ]
    vectors = [v.reshape(-1, 128) for v in (attn_gain, ffn_gain, mix_gate)]
    return pl.pallas_call(
        lambda *refs: prep_kernel(
            *refs, capacity=capacity, ep_count=ep_count, tp_count=tp_count
        ),
        out_shape=[pltpu.VMEM(s, d) for s, d in outs],
        in_specs=[HB] * 14,
        out_specs=[VM] * len(outs),
        scratch_shapes=[
            pltpu.SMEM(lengths.shape, jnp.int32),
            pltpu.SMEM(forget_bias.shape, f32),
            pltpu.VMEM((3,) + vectors[0].shape, bf16),
            pltpu.VMEM((2, tok), jnp.int32),
            pltpu.VMEM((2, tok), f32),
            pltpu.VMEM(cum_gate.shape, f32),
            pltpu.SemaphoreType.DMA((14,)),
        ],
        compiler_params=params(12),
        name="prep",
    )(
        *stay(
            lengths, forget_bias, *vectors, chosen.T, route_weight.T, cum_gate, kv_cache, w_query,
            w_key.T, w_value.T, w_forget.T, w_out,
        )
    )


def block_at(here, count, k, part):
    return pl.multiple_of(lax.rem(here + (count - k), count) * part, part)


def attend_kernel(kv_ref, wq_ref, wkv_ref, wf_ref, wo_ref, bias_ref, gains_ref, *rest):
    count = len(rest) - 7
    x_refs, (out_ref, q_scr, e_scr, p_scr, o_scr, s_scr, w_scr) = rest[:count], rest[count:]
    tok, part = x_refs[0].shape
    group = wf_ref.shape[0]
    cache = kv_ref.shape[1]
    pack = 8 // group
    rows = pack * group
    here = lax.axis_index("tp")
    xs = [r[...].astype(f32) for r in x_refs]
    square = sum(jnp.sum(x * x, axis=1, keepdims=True) for x in xs) * (1.0 / (part * count))
    inv = lax.rsqrt(square + epsilon)
    q = kv_new = forget = None
    for k, x in enumerate(xs):
        at = block_at(here, count, k, part)
        h = (x * inv * gains_ref[0:1, pl.ds(at, part)]).astype(bf16)
        a = jnp.dot(h, wq_ref[pl.ds(at, part), :], preferred_element_type=f32)
        b = lax.dot_general(h, wkv_ref[:, pl.ds(at, part)], NT, preferred_element_type=f32)
        c = lax.dot_general(h, wf_ref[:, pl.ds(at, part)], NT, preferred_element_type=f32)
        q, kv_new, forget = (a, b, c) if k == 0 else (q + a, kv_new + b, forget + c)
    q = q.astype(bf16).astype(f32)
    kv_new = kv_new.astype(bf16).astype(f32)
    forget = forget + gains_ref[3:4, 0:group]
    forget = jnp.minimum(forget, 0.0) - jnp.log1p(jnp.exp(-jnp.abs(forget)))
    scale = HD ** (-0.5)
    lane = lax.broadcasted_iota(jnp.int32, (tok, 2 * HD), 1)
    for g in range(group):
        qg = q[:, g * HD:(g + 1) * HD]
        own = jnp.sum(qg * kv_new[:, :HD], axis=1, keepdims=True) * scale
        q_scr[pl.ds(g, tok, stride=group), :] = jnp.concatenate([qg * scale, jnp.zeros_like(qg)], axis=1)
        e_scr[pl.ds(g, tok, stride=group), :] = jnp.where(lane == 0, forget[:, g:g + 1], own)
    row = lax.broadcasted_iota(jnp.int32, (rows, cache), 0)
    small = lax.broadcasted_iota(jnp.int32, (rows, 2 * HD), 0)
    for b in range(tok // pack):
        part_rows = slice(b * rows, (b + 1) * rows)
        qb = q_scr[part_rows, :].astype(bf16)
        s = lax.dot_general(qb, kv_ref[b * pack], NT, preferred_element_type=f32)
        for j in range(1, pack):
            sj = lax.dot_general(qb, kv_ref[b * pack + j], NT, preferred_element_type=f32)
            s = jnp.where(row < j * group, s, sj)
        s_scr[part_rows, :] = s + bias_ref[part_rows, :]
    extra = e_scr[...]
    own = extra[:, 1:2] - extra[:, 0:1]
    s = s_scr[...]
    top = jnp.maximum(jnp.max(s, axis=1, keepdims=True), own)
    w = jnp.exp(s - top)
    own_w = jnp.exp(own - top)
    scale_back = 1.0 / (jnp.sum(w, axis=1, keepdims=True) + own_w)
    w_scr[...] = (w * scale_back).astype(bf16)
    p_scr[...] = jnp.broadcast_to((own_w * scale_back).astype(bf16).astype(f32), p_scr.shape)
    for b in range(tok // pack):
        part_rows = slice(b * rows, (b + 1) * rows)
        p = w_scr[part_rows, :]
        o = jnp.dot(p, kv_ref[b * pack], preferred_element_type=f32)
        for j in range(1, pack):
            oj = jnp.dot(p, kv_ref[b * pack + j], preferred_element_type=f32)
            o = jnp.where(small < j * group, o, oj)
        o_scr[part_rows, :] = o
    heads = []
    for g in range(group):
        o = o_scr[pl.ds(g, tok, stride=group), :] + p_scr[pl.ds(g, tok, stride=group), :] * kv_new
        heads.append(o[:, HD:].astype(bf16))
    head_out = jnp.concatenate(heads, axis=1)
    out_ref[...] = jnp.dot(head_out, wo_ref[...], preferred_element_type=f32).astype(bf16)


def attend(xs, kv, wq, wkv, wf, wo, bias, gains):
    tok = xs[0].shape[0]
    scr = pltpu.VMEM((bias.shape[0], 2 * HD), f32)
    return pl.pallas_call(
        attend_kernel,
        out_shape=jax.ShapeDtypeStruct((tok, wo.shape[1]), bf16),
        in_specs=[VM] * (7 + len(xs)),
        out_specs=VM,
        scratch_shapes=[scr] * 4 + [pltpu.VMEM(bias.shape, f32), pltpu.VMEM(bias.shape, bf16)],
        compiler_params=params(12),
        name="attend",
    )(kv, wq, wkv, wf, wo, bias, gains, *xs)


def mid_kernel(gains_ref, send_ref, *rest):
    count = (len(rest) - 3) // 2
    x_refs, p_refs = rest[:count], rest[count : 2 * count]
    h_ref, res_ref, go_ref = rest[2 * count :]
    part = x_refs[0].shape[1]
    here = lax.axis_index("tp")
    square = 0.0
    blocks = []
    for k in range(count):
        at = block_at(here, count, k, part)
        total = sum(p[:, pl.ds(at, part)].astype(f32) for p in p_refs)
        block = (x_refs[k][...].astype(f32) + total).astype(bf16)
        if k == 0:
            res_ref[...] = block
        block = block.astype(f32)
        square = square + jnp.sum(block * block, axis=1, keepdims=True)
        blocks.append((at, block))
    inv = lax.rsqrt(square * (1.0 / (part * count)) + epsilon)
    for at, block in blocks:
        h = (block * inv * gains_ref[1:2, pl.ds(at, part)]).astype(bf16)
        h_ref[:, pl.ds(at, part)] = h
        go_ref[:, pl.ds(at, part)] = jnp.dot(
            send_ref[...], h, preferred_element_type=f32
        ).astype(bf16)


def middle(gains, send, xs, parts):
    tok, part = xs[0].shape
    width = parts[0].shape[1]
    return pl.pallas_call(
        mid_kernel,
        out_shape=[
            jax.ShapeDtypeStruct((tok, width), bf16),
            jax.ShapeDtypeStruct((tok, part), bf16),
            jax.ShapeDtypeStruct((send.shape[0], width), bf16),
        ],
        in_specs=[VM] * (2 + 2 * len(xs)),
        out_specs=[VM] * 3,
        compiler_params=params(6),
        name="middle",
    )(gains, send, *xs, *parts)


def silu(a):
    return a / (1.0 + jnp.exp(-a))


def dense_kernel(h_ref, gains_ref, wg_hbm, wu_hbm, wd_hbm, *rest):
    count = len(rest) - 5
    out_refs, (blend_ref, wg_ref, wu_ref, wd_ref, sems) = rest[:count], rest[count:]
    moves = [(wg_hbm, wg_ref), (wu_hbm, wu_ref), (wd_hbm, wd_ref)]
    copies = [pltpu.make_async_copy(a, b, sems.at[i]) for i, (a, b) in enumerate(moves)]
    for c in copies:
        c.start()
    h = h_ref[...]
    blend = jnp.sum(h.astype(f32) * gains_ref[2:3, :], axis=1, keepdims=True)
    blend_ref[...] = jnp.broadcast_to(1.0 / (1.0 + jnp.exp(-blend)), blend_ref.shape)
    copies[0].wait()
    a = jnp.dot(h, wg_ref[...], preferred_element_type=f32)
    copies[1].wait()
    b = jnp.dot(h, wu_ref[...], preferred_element_type=f32)
    hidden = (silu(a) * b).astype(bf16)
    copies[2].wait()
    here = lax.axis_index("tp")
    part = out_refs[0].shape[1]
    for k in range(count):
        at = pl.multiple_of(lax.rem(here + k, count) * part, part)
        y = jnp.dot(hidden, wd_ref[:, pl.ds(at, part)], preferred_element_type=f32)
        out_refs[k][...] = y.astype(bf16)


def dense(h_two, gains, wg, wu, wd, count):
    tok = h_two.shape[0]
    part = wd.shape[1] // count
    return pl.pallas_call(
        dense_kernel,
        out_shape=[jax.ShapeDtypeStruct((tok, part), bf16)] * count
        + [jax.ShapeDtypeStruct((tok, 128), f32)],
        in_specs=[VM] * 2 + [HB] * 3,
        out_specs=[VM] * (count + 1),
        scratch_shapes=[
            pltpu.VMEM(wg.shape, bf16),
            pltpu.VMEM(wu.shape, bf16),
            pltpu.VMEM(wd.shape, bf16),
            pltpu.SemaphoreType.DMA((3,)),
        ],
        compiler_params=params(8),
        name="dense",
    )(h_two, gains, *stay(wg, wu, wd))


def expert_kernel(x_ref, wg_ref, wu_ref, wd_ref, out_ref):
    x = x_ref[...]
    a = jnp.dot(x, wg_ref[...], preferred_element_type=f32)
    b = jnp.dot(x, wu_ref[...], preferred_element_type=f32)
    hidden = (silu(a) * b).astype(bf16)
    y = jnp.dot(hidden, wd_ref[...], preferred_element_type=f32).astype(bf16)
    cap, width = out_ref.shape[2:]
    for t in range(out_ref.shape[1]):
        out_ref[:, t] = y[:, t * width : (t + 1) * width].reshape(-1, cap, width)


def expert(x, wg, wu, wd, ep_count, tp_count, capacity):
    return pl.pallas_call(
        expert_kernel,
        out_shape=jax.ShapeDtypeStruct(
            (ep_count, tp_count, capacity, wd.shape[1] // tp_count), bf16
        ),
        in_specs=[VM] * 4,
        out_specs=VM,
        compiler_params=params(8),
        name="expert",
    )(x, wg, wu, wd)


def final_kernel(take_ref, back_ref, res_ref, blend_ref, *rest):
    d_refs, out_ref = rest[:-1], rest[-1]
    tok = res_ref.shape[0]
    both = jnp.dot(take_ref[...], back_ref[...], preferred_element_type=f32)
    routed = both[:tok] + both[tok:]
    dense_out = sum(d[...].astype(f32) for d in d_refs)
    out_ref[...] = (res_ref[...].astype(f32) + routed + blend_ref[:, 0:1] * dense_out).astype(bf16)


def final(take, back, res, blend, parts):
    return pl.pallas_call(
        final_kernel,
        out_shape=jax.ShapeDtypeStruct(res.shape, bf16),
        in_specs=[VM] * (4 + len(parts)),
        out_specs=VM,
        compiler_params=params(6),
        name="final",
    )(take, back, res, blend, *parts)


def ring(value, axis):
    count = lax.axis_size(axis)
    return [value] + [
        lax.ppermute(value, axis, [(i, (i + k) % count) for i in range(count)])
        for k in range(1, count)
    ]


def local(
    tokens,
    kv_cache,
    cum_gate,
    lengths,
    w_query,
    w_key,
    w_value,
    w_forget,
    forget_bias,
    w_out,
    attn_gain,
    ffn_gain,
    mix_gate,
    expert_gate,
    expert_up,
    expert_down,
    chosen,
    route_weight,
    dense_gate,
    dense_up,
    dense_down,
):
    tok_count, slice_width = tokens.shape
    ep_count = lax.axis_size("ep")
    tp_count = lax.axis_size("tp")
    capacity = max(2, (4 * tok_count + ep_count - 1) // ep_count)
    xs = ring(tokens, "tp")
    kv, wq, wkv, wf, wo, bias, gains, send, take = prep(
        tokens, kv_cache, cum_gate, lengths, w_query, w_key, w_value, w_forget, forget_bias,
        w_out, attn_gain, ffn_gain, mix_gate, chosen, route_weight, capacity, ep_count, tp_count,
    )
    partial_value = attend(xs, kv, wq, wkv, wf, wo, bias, gains)
    h_two, residual, outgoing = middle(gains, send, xs, ring(partial_value, "tp"))
    model_width = h_two.shape[1]
    outgoing = outgoing.reshape(ep_count, capacity, model_width)
    received = lax.all_to_all(outgoing, "ep", split_axis=0, concat_axis=0, tiled=True)
    *dense_parts, blend = dense(h_two, gains, dense_gate, dense_up, dense_down, tp_count)
    parts = expert(
        received.reshape(-1, model_width), expert_gate[0], expert_up[0], expert_down[0],
        ep_count, tp_count, capacity,
    )
    parts = parts.reshape(ep_count * tp_count, capacity, slice_width)
    returned = lax.all_to_all(parts, ("ep", "tp"), split_axis=0, concat_axis=0, tiled=True)
    returned = returned.reshape(-1, slice_width)
    dense_sum = [dense_parts[0]] + [
        lax.ppermute(dense_parts[k], "tp", [(i, (i + k) % tp_count) for i in range(tp_count)])
        for k in range(1, tp_count)
    ]
    return final(take, returned, residual, blend, dense_sum)


def solution(mesh):
    in_specs = (
        P("ep", "tp"),
        P("ep", None, "tp"),
        P("ep", "tp", None),
        P("ep"),
        P(None, "tp"),
        P(None, "tp"),
        P(None, "tp"),
        P(None, "tp"),
        P("tp"),
        P("tp", None),
        P(),
        P(),
        P(),
        P("ep", None, "tp"),
        P("ep", None, "tp"),
        P("ep", "tp", None),
        P("ep", None),
        P("ep", None),
        P(None, "tp"),
        P(None, "tp"),
        P("tp", None),
    )
    out_specs = P("ep", "tp")
    return jax.shard_map(local, mesh=mesh, in_specs=in_specs, out_specs=out_specs, check_vma=False)
```
